32 devices in a mesh: sp: 8 (over z, x), tp: 4 (over y, core).
Axes of the slice: x: 2, y: 2, z: 4, core: 2. Of those that a mesh axis runs over, the one named last changes fastest.
Arguments:
- residual: bfloat16 [4096, 2048], P(('sp', 'tp')), may hold values from -6 to 6
- query_small: bfloat16 [4096, 8, 128], P('sp', 'tp'), may hold values from -120 to 120
- key_small: bfloat16 [4096, 8, 128], P('sp', 'tp'), may hold values from -6 to 6
- value_small: bfloat16 [4096, 8, 128], P('sp', 'tp'), may hold values from -6 to 6
- query_large: bfloat16 [4096, 8, 256], P('sp', 'tp'), may hold values from -120 to 120
- key_large: bfloat16 [4096, 8, 256], P('sp', 'tp'), may hold values from -6 to 6
- value_large: bfloat16 [4096, 8, 128], P('sp', 'tp'), may hold values from -6 to 6
- lambda_small: float32 [8], P('tp'), may hold values from 0.3 to 0.8
- lambda_large: float32 [8], P('tp'), may hold values from 0.3 to 0.8
- head_gain: float32 [128], replicated, may hold values from 0.1 to 1.9
- output_small: bfloat16 [1024, 2048], P('tp'), may hold values from -0.125 to 0.125
- output_large: bfloat16 [1024, 2048], P('tp'), may hold values from -0.125 to 0.125
- norm_gain: float32 [2048], replicated, may hold values from 0.1 to 1.9
- gate_weight: bfloat16 [2048, 5632], P('sp', 'tp'), may hold values from -0.125 to 0.125
- up_weight: bfloat16 [2048, 5632], P('sp', 'tp'), may hold values from -0.125 to 0.125
- down_weight: bfloat16 [5632, 2048], P('tp', 'sp'), may hold values from -0.3125 to 0.3125
Outputs:
- block_output: bfloat16 [4096, 2048], P(('sp', 'tp'))
The draws below stay inside these ranges and needn't reach their ends.
All inputs are finite; a program needn't handle non-finite values.
Results may differ from the reference program's by a relative error of at most 0.015.
Values may be sent and summed in bfloat16 or wider, within the bound.
A program may use at most 128 MiB of HBM per device.

```python
import math
import jax
import jax.numpy as jnp
from jax import lax

D = 2048
HA = 8
HB = 8
KA = 64
KB = 128
VD = 128
FF = 5632
SEQ = 4096


def draw_pair(key, head_count, width, salt):
    base = jax.random.fold_in(key, salt)
    key_draw, query_draw = jax.random.split(base, 2)
    key_rows = jnp.clip(1.3 * jax.random.normal(key_draw, (SEQ, head_count, width), jnp.float32), -6.0, 6.0)
    query_rows = jnp.clip(1.3 * jax.random.normal(query_draw, (SEQ, head_count, width), jnp.float32), -6.0, 6.0)
    return (query_rows, key_rows)


def draw_query_small(key, part):
    return draw_pair(key, HA, 2 * KA, 11)[0].astype(jnp.bfloat16)


def draw_key_small(key, part):
    return draw_pair(key, HA, 2 * KA, 11)[1].astype(jnp.bfloat16)


def draw_query_large(key, part):
    return draw_pair(key, HB, 2 * KB, 23)[0].astype(jnp.bfloat16)


def draw_key_large(key, part):
    return draw_pair(key, HB, 2 * KB, 23)[1].astype(jnp.bfloat16)


def block_levels(key, shape, shards, least, largest):
    def one(position, blocks):
        heights = jax.random.uniform(jax.random.fold_in(jax.random.fold_in(key, 6), position), (blocks,), jnp.float32, least / len(shards), largest / len(shards))
        return jnp.repeat(jnp.exp(heights), shape[position] // blocks).reshape((-1,) + (1,) * (len(shape) - position - 1))

    factor_of = one(*shards[0])
    for cut in shards[1:]:
        factor_of = factor_of * one(*cut)
    return factor_of


def scatter_about(key, shape, scale, bound, shards=(), kind=jnp.bfloat16):
    values = jax.random.normal(key, shape, jnp.float32) * scale
    if len(shards) > 0:
        values = block_levels(key, shape, shards, -0.22, 0.18) * values
    return jnp.clip(values, min=-bound, max=bound).astype(kind)


def setup_inputs(seed: int = 0) -> dict:
    key_list = jax.random.split(jax.random.key(seed), 17)
    return {
        "residual": scatter_about(key_list[0], (SEQ, D), 1.0, 6.0, ((0, 32),)),
        "query_small": draw_query_small(jax.random.fold_in(key_list[16], 71), 0),
        "key_small": draw_key_small(jax.random.fold_in(key_list[16], 71), 0),
        "value_small": scatter_about(key_list[3], (SEQ, HA, VD), 1.0, 6.0, ((0, 8), (1, 4))),
        "query_large": draw_query_large(jax.random.fold_in(key_list[16], 71), 0),
        "key_large": draw_key_large(jax.random.fold_in(key_list[16], 71), 0),
        "value_large": scatter_about(key_list[6], (SEQ, HB, VD), 1.0, 6.0, ((0, 8), (1, 4))),
        "lambda_small": jnp.clip(0.3 + 0.5 * jax.random.uniform(key_list[7], (HA,), jnp.float32) ** block_levels(key_list[7], (HA,), ((0, 4),), -0.2, 0.2), 0.3, 0.8),
        "lambda_large": jnp.clip(0.3 + 0.5 * jax.random.uniform(key_list[8], (HB,), jnp.float32) ** block_levels(key_list[8], (HB,), ((0, 4),), -0.2, 0.2), 0.3, 0.8),
        "head_gain": jnp.clip(1.0 + 0.18 * jax.random.normal(key_list[9], (VD,), jnp.float32), 0.1, 1.9),
        "output_small": scatter_about(key_list[10], (HA * VD, D), ((HA + HB) * VD) ** -0.5, 0.125, ((0, 4),)),
        "output_large": scatter_about(key_list[11], (HB * VD, D), ((HA + HB) * VD) ** -0.5, 0.125, ((0, 4),)),
        "norm_gain": jnp.clip(1.0 + 0.18 * jax.random.normal(key_list[12], (D,), jnp.float32), 0.1, 1.9),
        "gate_weight": scatter_about(key_list[13], (D, FF), D ** -0.5, 0.125, ((0, 8), (1, 4))),
        "up_weight": scatter_about(key_list[14], (D, FF), D ** -0.5, 0.125, ((0, 8), (1, 4))),
        "down_weight": scatter_about(key_list[15], (FF, D), (FF // 16) ** -0.5, 0.3125, ((0, 4), (1, 8))),
    }


residual_scale = 8.0 ** 0.25
branch_scale = 0.8
norm_epsilon = 1e-05
masked_score = -1e+30

def head_group(queries, key_rows, values, lambdas, head_gain):
    length, head_count, doubled = queries.shape
    head_size = doubled // 2
    score_scale = head_size ** (-0.5)
    query_maps = queries.reshape(length, head_count, 2, head_size).astype(jnp.float32)
    key_maps = key_rows.reshape(length, head_count, 2, head_size).astype(jnp.float32)
    value_rows = values.astype(jnp.float32)
    block_size = math.gcd(length, 256)
    key_index = jnp.arange(length, dtype=jnp.int32)

    def one_block(block_index):
        offset = block_index * block_size
        query_block = lax.dynamic_slice_in_dim(query_maps, offset, block_size, 0)
        scores = jnp.einsum('qhmd,khmd->hmqk', query_block, key_maps) * score_scale
        query_index = offset + jnp.arange(block_size, dtype=jnp.int32)
        visible = key_index[None, :] <= query_index[:, None]
        scores = jnp.where(visible, scores, masked_score)
        highest = lax.optimization_barrier(jnp.max(scores, axis=-1, keepdims=True))
        weights = jnp.where(visible, jnp.exp(scores - highest), 0.0)
        totals = lax.optimization_barrier(jnp.sum(weights, axis=-1))
        rounded = lax.optimization_barrier(weights.astype(jnp.bfloat16)).astype(jnp.float32)
        map_out = jnp.einsum('hmqk,khe->hmqe', rounded, value_rows) / totals[..., None]
        combined = map_out[:, 0] - lambdas[:, None, None] * map_out[:, 1]
        mean_square = lax.optimization_barrier(jnp.mean(combined * combined, axis=-1, keepdims=True))
        normed = combined * lax.rsqrt(mean_square + norm_epsilon) * head_gain * branch_scale
        return jnp.transpose(normed, (1, 0, 2)).astype(jnp.bfloat16)
    blocks = lax.map(one_block, jnp.arange(length // block_size, dtype=jnp.int32))
    return blocks.reshape(length, head_count * values.shape[2])

def layer_norm(values, gains):
    centered = values - lax.optimization_barrier(jnp.mean(values, axis=-1, keepdims=True))
    variance = lax.optimization_barrier(jnp.mean(centered * centered, axis=-1, keepdims=True))
    return centered * lax.rsqrt(variance + norm_epsilon) * gains

def reference(residual, query_small, key_small, value_small, query_large, key_large, value_large, lambda_small, lambda_large, head_gain, output_small, output_large, norm_gain, gate_weight, up_weight, down_weight):
    attended_small = head_group(query_small, key_small, value_small, lambda_small, head_gain)
    attended_large = head_group(query_large, key_large, value_large, lambda_large, head_gain)
    mixed_sum = jnp.dot(attended_small, output_small, preferred_element_type=jnp.float32) + jnp.dot(attended_large, output_large, preferred_element_type=jnp.float32)
    pre_norm = residual_scale * residual.astype(jnp.float32) + mixed_sum
    normed = layer_norm(pre_norm, norm_gain).astype(jnp.bfloat16)
    gate_rows = jnp.dot(normed, gate_weight, preferred_element_type=jnp.float32)
    up_rows = jnp.dot(normed, up_weight, preferred_element_type=jnp.float32)
    hidden = (jax.nn.silu(gate_rows) * up_rows).astype(jnp.bfloat16)
    down_sum = jnp.dot(hidden, down_weight, preferred_element_type=jnp.float32)
    return (residual_scale * normed.astype(jnp.float32) + 0.5 * down_sum).astype(jnp.bfloat16)
```

```python
import functools

import jax
import jax.numpy as jnp
from jax import lax
from jax.experimental import pallas as pl
from jax.experimental.pallas import tpu as pltpu
from jax.sharding import PartitionSpec as P

residual_scale = 8.0**0.25
branch_scale = 0.8
norm_epsilon = 1e-05
masked_score = -1e30
log2_e = 1.4426950408889634


def layer_norm(values, gains):
    centered = values - jnp.mean(values, axis=-1, keepdims=True)
    variance = jnp.mean(centered * centered, axis=-1, keepdims=True)
    return centered * lax.rsqrt(variance + norm_epsilon) * gains


def fold_lanes(values, op):
    result = values[:, :128]
    for start in range(128, values.shape[1], 128):
        result = op(result, values[:, start : start + 128])
    return result


def attend_kernel(rows, owners, lambdas, q_ref, k_ref, v_ref, gain_ref, o_ref, scores, peak, total, acc):
    slots, tokens, doubled = k_ref.shape
    size = doubled // 2
    factor = size**-0.5 * log2_e
    me = owners[0]
    lam = lambdas[pl.program_id(0)]
    last = (((1,), (1,)), ((), ()))
    for start in range(0, tokens, rows):
        outs = []
        for which in range(2):
            if size % 128 == 0:
                lanes = slice(which * size, (which + 1) * size)
                query = q_ref[start : start + rows, lanes]
            else:
                lanes = slice(0, doubled)
                query = q_ref[start : start + rows, :]
                lane = lax.broadcasted_iota(jnp.int32, query.shape, 1)
                query = jnp.where((lane >= size) == (which == 1), query, jnp.zeros_like(query))

            def score(slot):
                return lax.dot_general(
                    query, k_ref[slot, :, lanes], last, preferred_element_type=jnp.float32
                )

            near = score(0)
            row = start + lax.broadcasted_iota(jnp.int32, near.shape, 0)
            column = lax.broadcasted_iota(jnp.int32, near.shape, 1)
            near = jnp.where(column <= row, near, masked_score)
            scores[0] = near
            peak[...] = fold_lanes(near, jnp.maximum)

            @pl.loop(1, slots)
            def _(slot):
                @pl.when(owners[slot] < me)
                def _():
                    far = score(slot)
                    scores[slot] = far
                    peak[...] = jnp.maximum(peak[...], fold_lanes(far, jnp.maximum))

            highest = jnp.max(peak[...], axis=1, keepdims=True)
            weights = jnp.exp2((scores[0] - highest) * factor)
            total[...] = fold_lanes(weights, jnp.add)
            acc[...] = jnp.dot(
                weights.astype(jnp.bfloat16), v_ref[0], preferred_element_type=jnp.float32
            )

            @pl.loop(1, slots)
            def _(slot):
                @pl.when(owners[slot] < me)
                def _():
                    weights = jnp.exp2((scores[slot] - highest) * factor)
                    total[...] += fold_lanes(weights, jnp.add)
                    acc[...] += jnp.dot(
                        weights.astype(jnp.bfloat16), v_ref[slot], preferred_element_type=jnp.float32
                    )

            outs.append(acc[...] / jnp.sum(total[...], axis=1, keepdims=True))
        combined = outs[0] - lam * outs[1]
        mean_square = jnp.mean(combined * combined, axis=1, keepdims=True)
        normed = combined * lax.rsqrt(mean_square + norm_epsilon) * gain_ref[...] * branch_scale
        o_ref[start : start + rows, :] = normed.astype(o_ref.dtype)


def attend(owners, lambdas, queries, stacked, offset, heads, width, head_gain, name):
    slots, tokens, _ = stacked.shape
    doubled = queries.shape[1] // heads
    rows = min(256, tokens)
    key_at = offset // doubled
    value_at = (offset + heads * doubled) // width
    work = heads * 2 * tokens * slots * tokens
    return pl.pallas_call(
        functools.partial(attend_kernel, rows),
        out_shape=jax.ShapeDtypeStruct((tokens, heads * width), jnp.bfloat16),
        grid_spec=pltpu.PrefetchScalarGridSpec(
            num_scalar_prefetch=2,
            grid=(heads,),
            in_specs=[
                pl.BlockSpec((tokens, doubled), lambda h, *_: (0, h)),
                pl.BlockSpec((slots, tokens, doubled), lambda h, *_: (0, 0, key_at + h)),
                pl.BlockSpec((slots, tokens, width), lambda h, *_: (0, 0, value_at + h)),
                pl.BlockSpec((1, width), lambda h, *_: (0, 0)),
            ],
            out_specs=pl.BlockSpec((tokens, width), lambda h, *_: (0, h)),
            scratch_shapes=[
                pltpu.VMEM((slots, rows, tokens), jnp.float32),
                pltpu.VMEM((rows, 128), jnp.float32),
                pltpu.VMEM((rows, 128), jnp.float32),
                pltpu.VMEM((rows, width), jnp.float32),
            ],
        ),
        compiler_params=pltpu.CompilerParams(vmem_limit_bytes=40 * 2**20),
        cost_estimate=pl.CostEstimate(
            flops=work * 512, bytes_accessed=stacked.size, transcendentals=work
        ),
        name=name,
    )(owners, lambdas, queries, stacked, stacked, head_gain.reshape(1, width))


def ring_gather(value):
    n = lax.axis_size("sp")
    order = list(range(0, n, 2)) + list(range(n - 1, 0, -2))
    forth = [(order[i], order[(i + 1) % n]) for i in range(n)]
    back = [(b, a) for a, b in forth]
    place = [0] * n
    for i, device in enumerate(order):
        place[device] = i
    position = jnp.array(place, jnp.int32)[lax.axis_index("sp")]
    table = jnp.array(order, jnp.int32)
    half = n // 2
    slots = [value]
    owners = [table[position]]
    ahead = behind = value
    split = value.shape[0] // 2
    for hop in range(1, half):
        ahead = lax.ppermute(ahead, "sp", forth)
        behind = lax.ppermute(behind, "sp", back)
        slots += [ahead, behind]
        owners += [table[(position - hop) % n], table[(position + hop) % n]]
    first = lax.ppermute(ahead[:split], "sp", forth)
    second = lax.ppermute(behind[split:], "sp", back)
    slots.append(jnp.concatenate([first, second], axis=0))
    owners.append(table[(position + half) % n])
    return slots, jnp.stack(owners)


def swap(value, axis, bit):
    pairs = [(i, i ^ (1 << bit)) for i in range(lax.axis_size(axis))]
    return lax.ppermute(value, axis, pairs)


def gather_rows(rows, bits):
    held = {0: rows}
    for bit in reversed(range(bits)):
        keys = sorted(held)
        sent = jnp.concatenate([held[k] for k in keys], axis=0) if len(keys) > 1 else held[0]
        got = swap(sent, "tp", bit)
        for i, k in enumerate(keys):
            held[k | (1 << bit)] = got[i * rows.shape[0] : (i + 1) * rows.shape[0]]
    return jnp.concatenate([held[k] for k in sorted(held)], axis=0)


def scatter_sum(values, bits):
    rows = values.shape[0] >> bits
    held = {k: values[k * rows : (k + 1) * rows] for k in range(1 << bits)}
    for bit in range(bits):
        kept = [k for k in sorted(held) if not k >> bit & 1]
        sent = [held[k | (1 << bit)].astype(jnp.bfloat16) for k in kept]
        got = swap(jnp.concatenate(sent, axis=0) if len(sent) > 1 else sent[0], "tp", bit)
        held = {
            k: held[k] + got[i * rows : (i + 1) * rows].astype(jnp.float32)
            for i, k in enumerate(kept)
        }
    return held[0]


def per_device(
    residual,
    query_small,
    key_small,
    value_small,
    query_large,
    key_large,
    value_large,
    lambda_small,
    lambda_large,
    head_gain,
    output_small,
    output_large,
    norm_gain,
    gate_weight,
    up_weight,
    down_weight,
):
    tokens, heads_small, _ = query_small.shape
    heads_large = query_large.shape[1]
    width = value_small.shape[2]
    rows = residual.shape[0]
    bits = lax.axis_size("tp").bit_length() - 1
    flat = [x.reshape(tokens, -1) for x in (key_small, value_small, key_large, value_large)]
    large_at = flat[0].shape[1] + flat[1].shape[1]
    slots, owners = ring_gather(jnp.concatenate(flat, axis=1))
    stacked = jnp.stack(slots)
    gate_full = lax.all_gather(gate_weight, "sp", axis=0, tiled=True)
    up_full = lax.all_gather(up_weight, "sp", axis=0, tiled=True)
    down_full = lax.all_gather(down_weight, "sp", axis=1, tiled=True)
    attended_small = attend(
        owners, lambda_small, query_small.reshape(tokens, -1), stacked, 0,
        heads_small, width, head_gain, "attend_small",
    )
    attended_large = attend(
        owners, lambda_large, query_large.reshape(tokens, -1), stacked, large_at,
        heads_large, width, head_gain, "attend_large",
    )
    attended = jnp.concatenate([attended_small, attended_large], axis=1)
    me = lax.axis_index("tp")
    attended = jnp.concatenate(
        [
            lax.dynamic_slice_in_dim(attended, (me ^ k) * rows, rows, 0)
            for k in range(1 << bits)
        ],
        axis=0,
    )
    output_weight = jnp.concatenate([output_small, output_large], axis=0)
    mixed_sum = scatter_sum(
        jnp.dot(attended, output_weight, preferred_element_type=jnp.float32), bits
    )
    normed = layer_norm(
        residual_scale * residual.astype(jnp.float32) + mixed_sum, norm_gain
    ).astype(jnp.bfloat16)
    whole_rows = gather_rows(normed, bits)
    gate_rows = jnp.dot(whole_rows, gate_full, preferred_element_type=jnp.float32)
    up_rows = jnp.dot(whole_rows, up_full, preferred_element_type=jnp.float32)
    hidden = (jax.nn.silu(gate_rows) * up_rows).astype(jnp.bfloat16)
    down_sum = scatter_sum(
        jnp.dot(hidden, down_full, preferred_element_type=jnp.float32), bits
    )
    return (residual_scale * normed.astype(jnp.float32) + 0.5 * down_sum).astype(jnp.bfloat16)


def solution(mesh):
    in_specs = (
        P(("sp", "tp"), None),
        P("sp", "tp", None),
        P("sp", "tp", None),
        P("sp", "tp", None),
        P("sp", "tp", None),
        P("sp", "tp", None),
        P("sp", "tp", None),
        P("tp"),
        P("tp"),
        P(),
        P("tp", None),
        P("tp", None),
        P(),
        P("sp", "tp"),
        P("sp", "tp"),
        P("tp", "sp"),
    )
    out_specs = P(("sp", "tp"), None)
    return jax.shard_map(
        per_device, mesh=mesh, in_specs=in_specs, out_specs=out_specs, check_vma=False
    )
```

```python
import functools

import jax
import jax.numpy as jnp
from jax import lax
from jax.experimental import pallas as pl
from jax.experimental.pallas import tpu as pltpu
from jax.sharding import PartitionSpec as P


residual_scale = 8.0**0.25
branch_scale = 0.8
norm_epsilon = 1e-05
masked_score = -1e30
log2_e = 1.4426950408889634


def layer_norm(values, gains):
    centered = values - jnp.mean(values, axis=-1, keepdims=True)
    variance = jnp.mean(centered * centered, axis=-1, keepdims=True)
    return centered * lax.rsqrt(variance + norm_epsilon) * gains


def fold_lanes(values, op):
    result = values[:, :128]
    for start in range(128, values.shape[1], 128):
        result = op(result, values[:, start : start + 128])
    return result


def attend_kernel(rows, owners, lambdas, q_ref, k_ref, v_ref, gain_ref, o_ref, scores, peak, total, acc):
    slots, tokens, doubled = k_ref.shape
    size = doubled // 2
    factor = size**-0.5 * log2_e
    me = owners[0]
    lam = lambdas[pl.program_id(0)]
    last = (((1,), (1,)), ((), ()))
    for start in range(0, tokens, rows):
        outs = []
        for which in range(2):
            if size % 128 == 0:
                lanes = slice(which * size, (which + 1) * size)
                query = q_ref[start : start + rows, lanes]
            else:
                lanes = slice(0, doubled)
                query = q_ref[start : start + rows, :]
                lane = lax.broadcasted_iota(jnp.int32, query.shape, 1)
                query = jnp.where((lane >= size) == (which == 1), query, jnp.zeros_like(query))

            def score(slot):
                return lax.dot_general(
                    query, k_ref[slot, :, lanes], last, preferred_element_type=jnp.float32
                )

            near = score(0)
            row = start + lax.broadcasted_iota(jnp.int32, near.shape, 0)
            column = lax.broadcasted_iota(jnp.int32, near.shape, 1)
            near = jnp.where(column <= row, near, masked_score)
            scores[0] = near
            peak[...] = fold_lanes(near, jnp.maximum)

            @pl.loop(1, slots)
            def _(slot):
                @pl.when(owners[slot] < me)
                def _():
                    far = score(slot)
                    scores[slot] = far
                    peak[...] = jnp.maximum(peak[...], fold_lanes(far, jnp.maximum))

            highest = jnp.max(peak[...], axis=1, keepdims=True)
            weights = jnp.exp2((scores[0] - highest) * factor)
            total[...] = fold_lanes(weights, jnp.add)
            acc[...] = jnp.dot(
                weights.astype(jnp.bfloat16), v_ref[0], preferred_element_type=jnp.float32
            )

            @pl.loop(1, slots)
            def _(slot):
                @pl.when(owners[slot] < me)
                def _():
                    weights = jnp.exp2((scores[slot] - highest) * factor)
                    total[...] += fold_lanes(weights, jnp.add)
                    acc[...] += jnp.dot(
                        weights.astype(jnp.bfloat16), v_ref[slot], preferred_element_type=jnp.float32
                    )

            outs.append(acc[...] / jnp.sum(total[...], axis=1, keepdims=True))
        combined = outs[0] - lam * outs[1]
        mean_square = jnp.mean(combined * combined, axis=1, keepdims=True)
        normed = combined * lax.rsqrt(mean_square + norm_epsilon) * gain_ref[...] * branch_scale
        o_ref[start : start + rows, :] = normed.astype(o_ref.dtype)


def attend(owners, lambdas, queries, stacked, offset, heads, width, head_gain):
    slots, tokens, _ = stacked.shape
    doubled = queries.shape[1] // heads
    rows = min(256, tokens)
    key_at = offset // doubled
    value_at = (offset + heads * doubled) // width
    work = heads * 2 * tokens * slots * tokens
    return pl.pallas_call(
        functools.partial(attend_kernel, rows),
        out_shape=jax.ShapeDtypeStruct((tokens, heads * width), jnp.bfloat16),
        grid_spec=pltpu.PrefetchScalarGridSpec(
            num_scalar_prefetch=2,
            grid=(heads,),
            in_specs=[
                pl.BlockSpec((tokens, doubled), lambda h, *_: (0, h)),
                pl.BlockSpec((slots, tokens, doubled), lambda h, *_: (0, 0, key_at + h)),
                pl.BlockSpec((slots, tokens, width), lambda h, *_: (0, 0, value_at + h)),
                pl.BlockSpec((1, width), lambda h, *_: (0, 0)),
            ],
            out_specs=pl.BlockSpec((tokens, width), lambda h, *_: (0, h)),
            scratch_shapes=[
                pltpu.VMEM((slots, rows, tokens), jnp.float32),
                pltpu.VMEM((rows, 128), jnp.float32),
                pltpu.VMEM((rows, 128), jnp.float32),
                pltpu.VMEM((rows, width), jnp.float32),
            ],
        ),
        compiler_params=pltpu.CompilerParams(vmem_limit_bytes=40 * 2**20),
        cost_estimate=pl.CostEstimate(
            flops=work * 512, bytes_accessed=stacked.size, transcendentals=work
        ),
    )(owners, lambdas, queries, stacked, stacked, head_gain.reshape(1, width))


def ring_gather(value, ties={}):
    n = lax.axis_size("sp")
    order = list(range(0, n, 2)) + list(range(n - 1, 0, -2))
    forth = [(order[i], order[(i + 1) % n]) for i in range(n)]
    back = [(b, a) for a, b in forth]
    place = [0] * n
    for i, device in enumerate(order):
        place[device] = i
    position = jnp.array(place, jnp.int32)[lax.axis_index("sp")]
    table = jnp.array(order, jnp.int32)
    half = n // 2
    slots = [value]
    owners = [table[position]]
    ahead = behind = value
    split = value.shape[0] // 2
    for hop in range(1, half):
        if hop in ties:
            ahead, behind, _ = lax.optimization_barrier((ahead, behind, ties[hop]))
        ahead = lax.ppermute(ahead, "sp", forth)
        behind = lax.ppermute(behind, "sp", back)
        slots += [ahead, behind]
        owners += [table[(position - hop) % n], table[(position + hop) % n]]
    first = lax.ppermute(ahead[:split], "sp", forth)
    second = lax.ppermute(behind[split:], "sp", back)
    slots.append(jnp.concatenate([first, second], axis=0))
    owners.append(table[(position + half) % n])
    return slots, jnp.stack(owners)


def swap(value, axis, bit):
    pairs = [(i, i ^ (1 << bit)) for i in range(lax.axis_size(axis))]
    return lax.ppermute(value, axis, pairs)


def gather_rows(rows, bits):
    held = {0: rows}
    for bit in reversed(range(bits)):
        keys = sorted(held)
        sent = jnp.concatenate([held[k] for k in keys], axis=0) if len(keys) > 1 else held[0]
        got = swap(sent, "tp", bit)
        for i, k in enumerate(keys):
            held[k | (1 << bit)] = got[i * rows.shape[0] : (i + 1) * rows.shape[0]]
    return jnp.concatenate([held[k] for k in sorted(held)], axis=0)


def scatter_sum(values, bits):
    rows = values.shape[0] >> bits
    held = {k: values[k * rows : (k + 1) * rows] for k in range(1 << bits)}
    for bit in range(bits):
        kept = [k for k in sorted(held) if not k >> bit & 1]
        sent = [held[k | (1 << bit)].astype(jnp.bfloat16) for k in kept]
        got = swap(jnp.concatenate(sent, axis=0) if len(sent) > 1 else sent[0], "tp", bit)
        held = {
            k: held[k] + got[i * rows : (i + 1) * rows].astype(jnp.float32)
            for i, k in enumerate(kept)
        }
    return held[0]


def per_device(
    residual,
    query_small,
    key_small,
    value_small,
    query_large,
    key_large,
    value_large,
    lambda_small,
    lambda_large,
    head_gain,
    output_small,
    output_large,
    norm_gain,
    gate_weight,
    up_weight,
    down_weight,
):
    tokens, heads_small, _ = query_small.shape
    heads_large = query_large.shape[1]
    width = value_small.shape[2]
    rows = residual.shape[0]
    bits = lax.axis_size("tp").bit_length() - 1
    flat = [x.reshape(tokens, -1) for x in (key_small, value_small, key_large, value_large)]
    large_at = flat[0].shape[1] + flat[1].shape[1]
    slots, owners = ring_gather(jnp.concatenate(flat, axis=1))
    stacked = jnp.stack(slots)
    gate_full = lax.all_gather(gate_weight, "sp", axis=0, tiled=True)
    up_full = lax.all_gather(up_weight, "sp", axis=0, tiled=True)
    attended_large = attend(
        owners, lambda_large, query_large.reshape(tokens, -1), stacked, large_at,
        heads_large, width, head_gain,
    )
    after_large, _ = lax.optimization_barrier((stacked, attended_large))
    attended_small = attend(
        owners, lambda_small, query_small.reshape(tokens, -1), after_large, 0,
        heads_small, width, head_gain,
    )
    attended = jnp.concatenate([attended_small, attended_large], axis=1)
    me = lax.axis_index("tp")
    attended = jnp.concatenate(
        [
            lax.dynamic_slice_in_dim(attended, (me ^ k) * rows, rows, 0)
            for k in range(1 << bits)
        ],
        axis=0,
    )
    output_weight = jnp.concatenate([output_small, output_large], axis=0)
    mixed_sum = scatter_sum(
        jnp.dot(attended, output_weight, preferred_element_type=jnp.float32), bits
    )
    normed = layer_norm(
        residual_scale * residual.astype(jnp.float32) + mixed_sum, norm_gain
    ).astype(jnp.bfloat16)
    whole_rows = gather_rows(normed, bits)
    ties = {1: slots[-1], 2: attended_large, 3: attended_small}
    down_slots, _ = ring_gather(down_weight, ties)
    down_ring = jnp.concatenate(down_slots, axis=1)
    gate_rows = jnp.dot(whole_rows, gate_full, preferred_element_type=jnp.float32)
    up_rows = jnp.dot(whole_rows, up_full, preferred_element_type=jnp.float32)
    hidden = (jax.nn.silu(gate_rows) * up_rows).astype(jnp.bfloat16)
    down_sum = scatter_sum(
        jnp.dot(hidden, down_ring, preferred_element_type=jnp.float32), bits
    )
    part = down_weight.shape[1]
    number = len(down_slots)
    down_sum = jnp.concatenate(
        [
            lax.dynamic_slice_in_dim(
                down_sum, jnp.sum(jnp.where(owners == c, jnp.arange(number), 0)) * part, part, 1
            )
            for c in range(number)
        ],
        axis=1,
    )
    return (residual_scale * normed.astype(jnp.float32) + 0.5 * down_sum).astype(jnp.bfloat16)


def solution(mesh):
    in_specs = (
        P(("sp", "tp"), None),
        P("sp", "tp", None),
        P("sp", "tp", None),
        P("sp", "tp", None),
        P("sp", "tp", None),
        P("sp", "tp", None),
        P("sp", "tp", None),
        P("tp"),
        P("tp"),
        P(),
        P("tp", None),
        P("tp", None),
        P(),
        P("sp", "tp"),
        P("sp", "tp"),
        P("tp", "sp"),
    )
    out_specs = P(("sp", "tp"), None)

    return jax.shard_map(
        per_device, mesh=mesh, in_specs=in_specs, out_specs=out_specs, check_vma=False
    )
```
